32 devices in a mesh: fs: 16 (over z, y, core), tp: 2 (over x).
Axes of the slice: x: 2, y: 2, z: 4, core: 2. Of those that a mesh axis runs over, the one named last changes fastest.
Arguments:
- inputs: bfloat16 [16384, 3072], P('fs'), may hold values from -6 to 6
- query_cot: bfloat16 [16384, 768], P('fs', 'tp'), may hold values from -0.046875 to 0.046875
- value_cot: bfloat16 [16384, 1536], P('fs', 'tp'), may hold values from -0.046875 to 0.046875
- query_factor: bfloat16 [3072, 192], P('fs'), may hold values from -0.109375 to 0.109375
- value_factor: bfloat16 [3072, 192], P('fs'), may hold values from -0.109375 to 0.109375
- query_weight: float32 [3072, 768], P('fs', 'tp'), may hold values from -0.109375 to 0.109375
- value_weight: float32 [3072, 1536], P('fs', 'tp'), may hold values from -0.109375 to 0.109375
- query_first: float32 [192, 768], P('fs', 'tp'), may hold values from -1.6 to 1.6
- query_second: float32 [192, 768], P('fs', 'tp'), may hold values from 0.002 to 0.05
- value_first: float32 [192, 1536], P('fs', 'tp'), may hold values from -1.6 to 1.6
- value_second: float32 [192, 1536], P('fs', 'tp'), may hold values from 0.002 to 0.05
Outputs:
- step_q: float32 [3072, 768], P('fs', 'tp')
- step_v: float32 [3072, 1536], P('fs', 'tp')
- new_q: float32 [3072, 768], P('fs', 'tp')
- new_v: float32 [3072, 1536], P('fs', 'tp')
- first_q: float32 [192, 768], P('fs', 'tp')
- second_q: float32 [192, 768], P('fs', 'tp')
- first_v: float32 [192, 1536], P('fs', 'tp')
- second_v: float32 [192, 1536], P('fs', 'tp')
- copy_q: bfloat16 [3072, 768], P(None, 'tp')
- copy_v: bfloat16 [3072, 1536], P(None, 'tp')
The draws below stay inside these ranges and needn't reach their ends.
All inputs are finite; a program needn't handle non-finite values.
Results may differ from the reference program's by a relative error of at most 0.0041.
Values may be sent and summed in bfloat16 or wider, within the bound.
A program may use at most 64 MiB of HBM per device.

```python
import math
import jax
import jax.numpy as jnp
from jax import lax

D = 3072
QW = 768
VW = 1536
R = 192
TOKENS = 16384


def draw_query_first(key, part):
    ramp = 1.0 + 3.0 * jnp.arange(R, dtype=jnp.float32)[:, None] / (R - 1)
    noise = jnp.clip(jax.random.normal(key, (R, QW), jnp.float32), -4.0, 4.0)
    return 0.1 * ramp * noise


def draw_value_first(key, part):
    ramp = 1.0 + 3.0 * jnp.arange(R, dtype=jnp.float32)[:, None] / (R - 1)
    noise = jnp.clip(jax.random.normal(key, (R, VW), jnp.float32), -4.0, 4.0)
    return 0.1 * ramp * noise


def steps_of(stream_key, dims, split, least, largest):
    gain = 1.0
    for axis_at, blocks in split:
        heights = jax.random.uniform(jax.random.fold_in(jax.random.fold_in(stream_key, 6), axis_at), (blocks,), jnp.float32, least / len(split), largest / len(split))
        gain = gain * jnp.repeat(jnp.exp(heights), dims[axis_at] // blocks).reshape((-1,) + (1,) * (len(dims) - 1 - axis_at))
    return gain


def centred(own_key, extent, width, bound, shards=(), kind=jnp.bfloat16):
    factor_of = steps_of(own_key, extent, shards, -0.22, 0.18) if shards else 1.0
    array = jax.random.normal(own_key, extent, jnp.float32) * width * factor_of
    return jnp.minimum(jnp.maximum(array, -bound), bound).astype(kind)


def setup_inputs(seed: int = 0) -> dict:
    streams_of = jax.random.split(jax.random.key(seed), 12)
    return {
        "inputs": centred(streams_of[0], (TOKENS, D), 1.0, 6.0, ((0, 16),)),
        "query_cot": centred(streams_of[1], (TOKENS, QW), (TOKENS ** -0.5), 0.046875, ((0, 16), (1, 2))),
        "value_cot": centred(streams_of[2], (TOKENS, VW), (TOKENS ** -0.5), 0.046875, ((0, 16), (1, 2))),
        "query_factor": centred(streams_of[3], (D, R), D ** -0.5, 0.109375, ((0, 16),)),
        "value_factor": centred(streams_of[4], (D, R), D ** -0.5, 0.109375, ((0, 16),)),
        "query_weight": centred(streams_of[5], (D, QW), D ** -0.5, 0.109375, ((0, 16), (1, 2)), jnp.float32),
        "value_weight": centred(streams_of[6], (D, VW), D ** -0.5, 0.109375, ((0, 16), (1, 2)), jnp.float32),
        "query_first": draw_query_first(jax.random.fold_in(streams_of[11], 71), 0),
        "query_second": jnp.clip(jnp.exp(math.log(0.05) - 3.218876 * jax.random.uniform(streams_of[8], (R, QW), jnp.float32) ** steps_of(streams_of[8], (R, QW), ((0, 16), (1, 2)), -0.2, 0.2)), 0.002, 0.05),
        "value_first": draw_value_first(jax.random.fold_in(streams_of[11], 71), 0),
        "value_second": jnp.clip(jnp.exp(math.log(0.05) - 3.218876 * jax.random.uniform(streams_of[10], (R, VW), jnp.float32) ** steps_of(streams_of[10], (R, VW), ((0, 16), (1, 2)), -0.2, 0.2)), 0.002, 0.05),
    }


first_decay = 0.9
second_decay = 0.99
small_eps = 1e-08
learn_rate = 0.01

def moments(old_first, old_second, gradient):
    first = first_decay * old_first + (1.0 - first_decay) * gradient
    second = second_decay * old_second + (1.0 - second_decay) * gradient * gradient
    unit = first / (jnp.sqrt(second) + small_eps)
    return (first, second, unit)

def reference(inputs, query_cot, value_cot, query_factor, value_factor, query_weight, value_weight, query_first, query_second, value_first, value_second):
    proj_q = jnp.dot(inputs, query_factor, preferred_element_type=jnp.float32).astype(jnp.bfloat16)
    proj_v = jnp.dot(inputs, value_factor, preferred_element_type=jnp.float32).astype(jnp.bfloat16)
    grad_q = jnp.dot(proj_q.T, query_cot, preferred_element_type=jnp.float32)
    grad_v = jnp.dot(proj_v.T, value_cot, preferred_element_type=jnp.float32)
    first_q, second_q, unit_q = moments(query_first, query_second, grad_q)
    first_v, second_v, unit_v = moments(value_first, value_second, grad_v)
    entries = float(unit_q.size + unit_v.size)
    step_scale = lax.rsqrt((jnp.sum(unit_q * unit_q) + jnp.sum(unit_v * unit_v)) / entries + 1e-06)
    bits_q = (step_scale * unit_q).astype(jnp.bfloat16)
    bits_v = (step_scale * unit_v).astype(jnp.bfloat16)
    step_q = jnp.dot(query_factor, bits_q, preferred_element_type=jnp.float32)
    step_v = jnp.dot(value_factor, bits_v, preferred_element_type=jnp.float32)
    new_q = query_weight - learn_rate * step_q
    new_v = value_weight - learn_rate * step_v
    return (step_q, step_v, new_q, new_v, first_q, second_q, first_v, second_v, new_q.astype(jnp.bfloat16), new_v.astype(jnp.bfloat16))
```

```python
import functools

import jax
import jax.numpy as jnp
from jax import lax
from jax.experimental import pallas as pl
from jax.experimental.pallas import tpu as pltpu
from jax.sharding import PartitionSpec as P

first_decay = 0.9
second_decay = 0.99
small_eps = 1e-08
learn_rate = 0.01
CORES = 2
COLS = 2


def moments(old_first, old_second, gradient):
    first = first_decay * old_first + (1.0 - first_decay) * gradient
    second = second_decay * old_second + (1.0 - second_decay) * gradient * gradient
    unit = first / (jnp.sqrt(second) + small_eps)
    return (first, second, unit)


class Place:
    def __init__(self, n, t):
        self.n, self.t = n, t
        self.depth = n // (COLS * CORES)
        self.me = lax.axis_index("fs")
        self.tp = lax.axis_index("tp")
        self.c = self.me % CORES
        self.y = (self.me // CORES) % COLS
        self.z = self.me // (CORES * COLS)

    def at(self, z, y, c):
        return (z * COLS + y) * CORES + c

    def up(self, k):
        return (self.z + k) % self.depth

    def down(self, k):
        return (self.z + self.depth - k) % self.depth


class Gather:
    def __init__(self, place, own, full, sems):
        self.p, self.own, self.full = place, own, full
        self.zs, self.zr, self.ys, self.yr, self.cs, self.cr = sems
        self.sent = []

    def _copy(self, src, slot, ss, rs, to):
        return pltpu.make_async_remote_copy(
            src_ref=src, dst_ref=self.full.at[slot], send_sem=ss, recv_sem=rs,
            device_id={"fs": to}, device_id_type=pl.DeviceIdType.MESH)

    def _go(self, copy):
        copy.start()
        self.sent.append(copy)

    def piece(self, k):
        slot = self.p.at(self.p.down(k), self.p.y, self.p.c)
        return slot, (self.own if k == 0 else self.full.at[slot])

    def send_z(self, k):
        p = self.p
        self._go(self._copy(self.own, p.me, self.zs.at[k], self.zr.at[k], p.at(p.up(k), p.y, p.c)))

    def wait_z(self, k):
        slot = self.p.at(self.p.down(k), self.p.y, self.p.c)
        self._copy(self.full.at[slot], slot, self.zs.at[k], self.zr.at[k], self.p.me).wait_recv()

    def send_yc(self, k):
        p = self.p
        slot, src = self.piece(k)
        self._go(self._copy(src, slot, self.ys.at[k], self.yr.at[k], p.at(p.z, 1 - p.y, p.c)))
        self._go(self._copy(src, slot, self.cs.at[0, k], self.cr.at[0, k], p.at(p.z, p.y, 1 - p.c)))

    def pass_y(self, k):
        p = self.p
        slot = p.at(p.down(k), 1 - p.y, p.c)
        got = self.full.at[slot]
        self._copy(got, slot, self.ys.at[k], self.yr.at[k], p.me).wait_recv()
        self._go(self._copy(got, slot, self.cs.at[1, k], self.cr.at[1, k], p.at(p.z, p.y, 1 - p.c)))

    def wait_c(self):
        p = self.p
        for j in range(2):
            for k in range(p.depth):
                slot = p.at(p.down(k), p.y if j == 0 else 1 - p.y, 1 - p.c)
                self._copy(self.full.at[slot], slot, self.cs.at[j, k], self.cr.at[j, k], p.me).wait_recv()

    def drain(self):
        for copy in self.sent:
            copy.wait_send()


def gather_sems(depth):
    dma = pltpu.SemaphoreType.DMA
    return [dma((depth,)), dma((depth,)), dma((depth,)), dma((depth,)), dma((2, depth)), dma((2, depth))]


def kernel(
    n, t, x_hbm, cq_hbm, cv_hbm, f_own, w_own, q1, q2, v1, v2,
    w_all, f_all, bits, first_q, second_q, first_v, second_v,
    x, cq, cv, g, gc_in, gs, gy_in, gt, gz_in, u_own, u_all, u_flat, sq, sq_in,
    acc_q, acc_v, local, gsem, tsem, *sems):
    p = Place(n, t)
    depth = p.depth
    rows = q1.shape[0]
    rank, q_cols = acc_q.shape
    v_cols = acc_v.shape[1]
    F = Gather(p, f_own, f_all, sems[0:6])
    W = Gather(p, w_own, w_all, sems[6:12])
    U = Gather(p, u_own, u_all, sems[12:18])
    loads = [
        pltpu.make_async_copy(x_hbm, x, local.at[0]),
        pltpu.make_async_copy(cq_hbm, cq, local.at[1]),
        pltpu.make_async_copy(cv_hbm, cv, local.at[2]),
    ]
    for copy in loads:
        copy.start()
    keep = pltpu.make_async_copy(w_own, w_all.at[p.me], local.at[3])
    keep.start()

    barrier = pltpu.get_barrier_semaphore()
    peers = [{"fs": p.at(p.up(k), p.y, p.c)} for k in range(1, depth)]
    peers += [{"fs": p.at(p.z, 1 - p.y, p.c)}, {"fs": p.at(p.z, p.y, 1 - p.c)}]
    peers += [{"tp": (p.tp + k) % t} for k in range(1, t)]
    for peer in peers:
        pl.semaphore_signal(barrier, inc=1, device_id=peer, device_id_type=pl.DeviceIdType.MESH)
    pl.semaphore_wait(barrier, len(peers))

    for k in range(1, depth):
        F.send_z(k)
    F.send_yc(0)
    f_all[p.me] = f_own[...]
    for k in range(1, depth):
        F.wait_z(k)
        F.send_yc(k)
    W.send_yc(0)
    W.send_z(1)
    for k in range(depth):
        F.pass_y(k)
    F.wait_c()
    for copy in loads:
        copy.wait()

    acc_q[...] = jnp.zeros_like(acc_q)
    acc_v[...] = jnp.zeros_like(acc_v)
    tile = 256

    @pl.loop(0, x.shape[0] // tile)
    def _(i):
        at = pl.ds(pl.multiple_of(i * tile, tile), tile)
        f = f_all[...].reshape(x.shape[1], 2 * rank)
        proj = jnp.dot(x[at, :], f, preferred_element_type=jnp.float32)
        turned = proj.T.astype(jnp.bfloat16)
        acc_q[...] += jnp.dot(turned[:rank], cq[at, :], preferred_element_type=jnp.float32)
        acc_v[...] += jnp.dot(turned[rank:], cv[at, :], preferred_element_type=jnp.float32)

    for j in range(n):
        c, y, z = j % CORES, (j // CORES) % COLS, j // (CORES * COLS)
        g[c, y, z, :, :q_cols] = acc_q[j * rows:(j + 1) * rows, :]
        g[c, y, z, :, q_cols:] = acc_v[j * rows:(j + 1) * rows, :]

    def swap(src, dst, k, peer):
        return pltpu.make_async_remote_copy(
            src_ref=src, dst_ref=dst, send_sem=gsem.at[0, k], recv_sem=gsem.at[1, k],
            device_id=peer, device_id_type=pl.DeviceIdType.MESH)

    to_core = swap(g.at[1 - p.c], gc_in, 0, {"fs": p.at(p.z, p.y, 1 - p.c)})
    to_core.start()
    to_core.wait()
    gs[...] = g[p.c] + gc_in[...]
    to_col = swap(gs.at[1 - p.y], gy_in, depth, {"fs": p.at(p.z, 1 - p.y, p.c)})
    to_col.start()
    W.wait_z(1)
    to_col.wait()
    gt[...] = gs[p.y] + gy_in[...]
    to_z = [swap(gt.at[p.up(k)], gz_in.at[k - 1], k, {"fs": p.at(p.up(k), p.y, p.c)}) for k in range(1, depth)]
    for copy in to_z:
        copy.start()
    W.send_yc(1)
    total = gt[p.z]
    for k, copy in enumerate(to_z):
        copy.wait()
        total = total + gz_in[k]
    a1, a2, uq = moments(q1[...], q2[...], total[:, :q_cols])
    b1, b2, uv = moments(v1[...], v2[...], total[:, q_cols:])
    u_own[:, :q_cols] = uq
    u_own[:, q_cols:] = uv
    for k in range(1, depth):
        U.send_z(k)
    U.send_yc(0)
    for k in range(2, depth):
        W.send_z(k)
    first_q[...] = a1
    second_q[...] = a2
    first_v[...] = b1
    second_v[...] = b2
    u_all[p.me] = u_own[...]
    for k in range(1, depth):
        U.wait_z(k)
        U.send_yc(k)
    for k in range(depth):
        U.pass_y(k)
    U.wait_c()
    for j in range(n):
        u_flat[j * rows:(j + 1) * rows, :] = u_all[j]
    own_sq = jnp.sum(u_flat[...] * u_flat[...])
    sq[...] = jnp.full(sq.shape, own_sq, jnp.float32)
    shares = [
        pltpu.make_async_remote_copy(
            src_ref=sq, dst_ref=sq_in.at[k - 1], send_sem=tsem.at[0, k], recv_sem=tsem.at[1, k],
            device_id={"tp": (p.tp + k) % t}, device_id_type=pl.DeviceIdType.MESH)
        for k in range(1, t)
    ]
    for copy in shares:
        copy.start()
    for k in range(2, depth):
        W.wait_z(k)
        W.send_yc(k)
    norm = sq[...]
    for k, copy in enumerate(shares):
        copy.wait()
        norm = norm + sq_in[k]
    entries = rank * (q_cols + v_cols) * t
    scale = lax.rsqrt(norm[:1, :1] / entries + 1e-06)
    bits[...] = (scale * u_flat[...]).astype(jnp.bfloat16)
    for k in range(depth):
        W.pass_y(k)
    W.wait_c()
    keep.wait()
    F.drain()
    U.drain()
    W.drain()


def exchange(inputs, query_cot, value_cot, f_own, w_own, query_first, query_second, value_first, value_second):
    n, t = lax.axis_size("fs"), lax.axis_size("tp")
    depth = n // (COLS * CORES)
    rows, q_cols = query_first.shape
    v_cols = value_first.shape[1]
    cols = q_cols + v_cols
    rank = rows * n
    any_, vmem = pl.BlockSpec(memory_space=pl.ANY), pl.BlockSpec(memory_space=pltpu.VMEM)
    f32, bf16 = jnp.float32, jnp.bfloat16
    dma = pltpu.SemaphoreType.DMA
    shape = jax.ShapeDtypeStruct
    return pl.pallas_call(
        functools.partial(kernel, n, t),
        out_shape=(
            shape((n,) + w_own.shape, bf16), shape((n,) + f_own.shape, bf16), shape((rank, cols), bf16),
            shape((rows, q_cols), f32), shape((rows, q_cols), f32),
            shape((rows, v_cols), f32), shape((rows, v_cols), f32),
        ),
        in_specs=[any_] * 3 + [vmem] * 6,
        out_specs=(any_,) + (vmem,) * 6,
        scratch_shapes=[
            pltpu.VMEM(inputs.shape, bf16), pltpu.VMEM(query_cot.shape, bf16), pltpu.VMEM(value_cot.shape, bf16),
            pltpu.VMEM((CORES, COLS, depth, rows, cols), f32), pltpu.VMEM((COLS, depth, rows, cols), f32),
            pltpu.VMEM((COLS, depth, rows, cols), f32), pltpu.VMEM((depth, rows, cols), f32),
            pltpu.VMEM((depth, rows, cols), f32), pltpu.VMEM((depth - 1, rows, cols), f32),
            pltpu.VMEM((rows, cols), f32), pltpu.VMEM((n, rows, cols), f32), pltpu.VMEM((rank, cols), f32),
            pltpu.VMEM((8, 128), f32), pltpu.VMEM((t - 1, 8, 128), f32),
            pltpu.VMEM((rank, q_cols), f32), pltpu.VMEM((rank, v_cols), f32),
            dma((4,)), dma((2, depth + 1)), dma((2, t)),
        ] + gather_sems(depth) * 3,
        compiler_params=pltpu.CompilerParams(
            collective_id=0, has_side_effects=True, vmem_limit_bytes=48 * 1024 * 1024),
    )(inputs, query_cot, value_cot, f_own, w_own, query_first, query_second, value_first, value_second)


def by_collectives(inputs, query_cot, value_cot, f_own, w_own, query_first, query_second, value_first, value_second):
    q_cols = query_cot.shape[1]
    n, rank = lax.axis_size("fs"), f_own.shape[1] // 2
    entries = rank * (q_cols + value_cot.shape[1]) * lax.axis_size("tp")
    f_all = lax.all_gather(f_own, "fs", axis=0)
    w_all = lax.all_gather(w_own, "fs", axis=0)
    proj = jnp.dot(inputs, f_all.reshape(-1, 2 * rank), preferred_element_type=jnp.float32).astype(jnp.bfloat16)
    over = (((0,), (0,)), ((), ()))
    term_q = lax.dot_general(proj[:, :rank], query_cot, over, preferred_element_type=jnp.float32)
    term_v = lax.dot_general(proj[:, rank:], value_cot, over, preferred_element_type=jnp.float32)
    own = lax.psum_scatter(jnp.concatenate([term_q, term_v], axis=1), "fs", scatter_dimension=0, tiled=True)
    first_q, second_q, unit_q = moments(query_first, query_second, own[:, :q_cols])
    first_v, second_v, unit_v = moments(value_first, value_second, own[:, q_cols:])
    total = lax.psum(jnp.sum(unit_q * unit_q) + jnp.sum(unit_v * unit_v), ("fs", "tp"))
    scale = lax.rsqrt(total / entries + 1e-06)
    mine = (scale * jnp.concatenate([unit_q, unit_v], axis=1)).astype(jnp.bfloat16)
    bits = lax.all_gather(mine, "fs", axis=0, tiled=True)
    return w_all, f_all, bits, first_q, second_q, first_v, second_v


def on_device(
    inputs, query_cot, value_cot, query_factor, value_factor, query_weight, value_weight,
    query_first, query_second, value_first, value_second,
):
    n = lax.axis_size("fs")
    rank, q_cols, v_cols = query_factor.shape[1], query_cot.shape[1], value_cot.shape[1]
    f_own = jnp.concatenate([query_factor, value_factor], axis=1)
    w_own = jnp.concatenate([query_weight, value_weight], axis=1).astype(jnp.bfloat16)
    whole = (
        n % (COLS * CORES) == 0 and n > COLS * CORES and lax.axis_size("tp") > 1 and q_cols % 128 == 0
        and v_cols % 128 == 0 and (2 * rank) % 128 == 0 and inputs.shape[1] % 128 == 0
        and inputs.shape[0] % 256 == 0 and query_factor.shape[0] % 16 == 0 and rank % 16 == 0
    )
    run = exchange if whole else by_collectives
    w_all, f_all, bits, first_q, second_q, first_v, second_v = run(
        inputs, query_cot, value_cot, f_own, w_own, query_first, query_second, value_first, value_second)
    f_full = f_all.reshape(-1, 2 * rank)
    w_full = w_all.reshape(-1, q_cols + v_cols)
    bits_q, bits_v = bits[:, :q_cols], bits[:, q_cols:]
    f32 = jnp.float32
    step_q = jnp.dot(query_factor, bits_q, preferred_element_type=f32)
    step_v = jnp.dot(value_factor, bits_v, preferred_element_type=f32)
    new_q = query_weight - learn_rate * step_q
    new_v = value_weight - learn_rate * step_v
    all_q = jnp.dot(f_full[:, :rank], bits_q, preferred_element_type=f32)
    all_v = jnp.dot(f_full[:, rank:], bits_v, preferred_element_type=f32)
    copy_q = (w_full[:, :q_cols].astype(f32) - learn_rate * all_q).astype(jnp.bfloat16)
    copy_v = (w_full[:, q_cols:].astype(f32) - learn_rate * all_v).astype(jnp.bfloat16)
    return (step_q, step_v, new_q, new_v, first_q, second_q, first_v, second_v, copy_q, copy_v)


def solution(mesh):
    row, both = P("fs", None), P("fs", "tp")
    in_specs = (row, both, both, row, row) + (both,) * 6
    out_specs = (both,) * 8 + (P(None, "tp"),) * 2
    return jax.shard_map(on_device, mesh=mesh, in_specs=in_specs, out_specs=out_specs, check_vma=False)
```

```python
import functools

import jax
import jax.numpy as jnp
from jax import lax
from jax.experimental import pallas as pl
from jax.experimental.pallas import tpu as pltpu
from jax.sharding import PartitionSpec as P

first_decay = 0.9
second_decay = 0.99
small_eps = 1e-08
learn_rate = 0.01
CORES = 2
COLS = 2


def moments(old_first, old_second, gradient):
    first = first_decay * old_first + (1.0 - first_decay) * gradient
    second = second_decay * old_second + (1.0 - second_decay) * gradient * gradient
    unit = first / (jnp.sqrt(second) + small_eps)
    return (first, second, unit)


class Place:
    def __init__(self, n, t):
        self.n, self.t = n, t
        self.depth = n // (COLS * CORES)
        self.me = lax.axis_index("fs")
        self.tp = lax.axis_index("tp")
        self.c = self.me % CORES
        self.y = (self.me // CORES) % COLS
        self.z = self.me // (CORES * COLS)

    def at(self, z, y, c):
        return (z * COLS + y) * CORES + c

    def up(self, k):
        return (self.z + k) % self.depth

    def down(self, k):
        return (self.z + self.depth - k) % self.depth


class Gather:
    def __init__(self, place, own, full, sems):
        self.p, self.own, self.full = place, own, full
        self.zs, self.zr, self.ys, self.yr, self.cs, self.cr = sems
        self.sent = []

    def _copy(self, src, slot, ss, rs, to):
        return pltpu.make_async_remote_copy(
            src_ref=src, dst_ref=self.full.at[slot], send_sem=ss, recv_sem=rs,
            device_id={"fs": to}, device_id_type=pl.DeviceIdType.MESH)

    def _go(self, copy):
        copy.start()
        self.sent.append(copy)

    def piece(self, k):
        slot = self.p.at(self.p.down(k), self.p.y, self.p.c)
        return slot, (self.own if k == 0 else self.full.at[slot])

    def send_z(self, k):
        p = self.p
        self._go(self._copy(self.own, p.me, self.zs.at[k], self.zr.at[k], p.at(p.up(k), p.y, p.c)))

    def wait_z(self, k):
        slot = self.p.at(self.p.down(k), self.p.y, self.p.c)
        self._copy(self.full.at[slot], slot, self.zs.at[k], self.zr.at[k], self.p.me).wait_recv()

    def send_yc(self, k):
        p = self.p
        slot, src = self.piece(k)
        self._go(self._copy(src, slot, self.ys.at[k], self.yr.at[k], p.at(p.z, 1 - p.y, p.c)))
        self._go(self._copy(src, slot, self.cs.at[0, k], self.cr.at[0, k], p.at(p.z, p.y, 1 - p.c)))

    def pass_y(self, k):
        p = self.p
        slot = p.at(p.down(k), 1 - p.y, p.c)
        got = self.full.at[slot]
        self._copy(got, slot, self.ys.at[k], self.yr.at[k], p.me).wait_recv()
        self._go(self._copy(got, slot, self.cs.at[1, k], self.cr.at[1, k], p.at(p.z, p.y, 1 - p.c)))

    def wait_c(self):
        p = self.p
        for j in range(2):
            for k in range(p.depth):
                slot = p.at(p.down(k), p.y if j == 0 else 1 - p.y, 1 - p.c)
                self._copy(self.full.at[slot], slot, self.cs.at[j, k], self.cr.at[j, k], p.me).wait_recv()

    def drain(self):
        for copy in self.sent:
            copy.wait_send()


def gather_sems(depth):
    dma = pltpu.SemaphoreType.DMA
    return [dma((depth,)), dma((depth,)), dma((depth,)), dma((depth,)), dma((2, depth)), dma((2, depth))]


class Line:
    def __init__(self, place, own, full, sems):
        self.p, self.own, self.full = place, own, full
        self.zs, self.zr, self.ys, self.yr, self.cs, self.cr = sems
        self.sent = []

    def _copy(self, src, slot, ss, rs, to):
        return pltpu.make_async_remote_copy(
            src_ref=src, dst_ref=self.full.at[slot], send_sem=ss, recv_sem=rs,
            device_id={"fs": to}, device_id_type=pl.DeviceIdType.MESH)

    def _go(self, when, make):
        pl.when(when)(lambda: make().start())
        self.sent.append((when, make))

    def origin(self, d, s):
        z = self.p.z - 1 - s if d == 0 else self.p.z + 1 + s
        return z, (z >= 0 if d == 0 else z < self.p.depth)

    def send(self, s):
        p = self.p
        for d in range(2):
            to, frm = (p.z + 1, p.z - s) if d == 0 else (p.z - 1, p.z + s)
            when = jnp.logical_and(to < p.depth, frm >= 0) if d == 0 else jnp.logical_and(to >= 0, frm < p.depth)

            def make(d=d, to=to, frm=frm):
                slot = p.at(frm, p.y, p.c)
                src = self.own if s == 0 else self.full.at[slot]
                return self._copy(src, slot, self.zs.at[d, s], self.zr.at[d, s], p.at(to, p.y, p.c))

            self._go(when, make)

    def wait(self, s):
        p = self.p
        for d in range(2):
            z, when = self.origin(d, s)

            @pl.when(when)
            def _(d=d, z=z):
                slot = p.at(z, p.y, p.c)
                self._copy(self.full.at[slot], slot, self.zs.at[d, s], self.zr.at[d, s], p.me).wait_recv()

    def own_yc(self):
        p, k = self.p, self.p.depth - 1
        self._go(True, lambda: self._copy(
            self.own, p.me, self.ys.at[0, k], self.yr.at[0, k], p.at(p.z, 1 - p.y, p.c)))
        self._go(True, lambda: self._copy(
            self.own, p.me, self.cs.at[0, 0, k], self.cr.at[0, 0, k], p.at(p.z, p.y, 1 - p.c)))

    def forward(self, d, s, also=True):
        p = self.p
        z, when = self.origin(d, s)
        when = jnp.logical_and(when, also)

        def to_y():
            slot = p.at(z, p.y, p.c)
            return self._copy(self.full.at[slot], slot, self.ys.at[d, s], self.yr.at[d, s], p.at(p.z, 1 - p.y, p.c))

        def to_c():
            slot = p.at(z, p.y, p.c)
            return self._copy(
                self.full.at[slot], slot, self.cs.at[0, d, s], self.cr.at[0, d, s], p.at(p.z, p.y, 1 - p.c))

        self._go(when, to_y)
        self._go(when, to_c)

    def items(self):
        last = self.p.depth - 1
        yield 0, last, self.p.z, True
        for s in range(last):
            for d in range(2):
                z, when = self.origin(d, s)
                yield d, s, z, when

    def pass_y(self):
        p = self.p
        for d, s, z, when in self.items():
            slot = p.at(z, 1 - p.y, p.c)

            @pl.when(when)
            def _(d=d, s=s, slot=slot):
                got = self.full.at[slot]
                self._copy(got, slot, self.ys.at[d, s], self.yr.at[d, s], p.me).wait_recv()

            self._go(when, lambda d=d, s=s, slot=slot: self._copy(
                self.full.at[slot], slot, self.cs.at[1, d, s], self.cr.at[1, d, s], p.at(p.z, p.y, 1 - p.c)))

    def wait_c(self):
        p = self.p
        for j in range(2):
            for d, s, z, when in self.items():
                slot = p.at(z, p.y if j == 0 else 1 - p.y, 1 - p.c)

                @pl.when(when)
                def _(d=d, s=s, slot=slot):
                    self._copy(self.full.at[slot], slot, self.cs.at[j, d, s], self.cr.at[j, d, s], p.me).wait_recv()

    def drain(self):
        for when, make in self.sent:
            pl.when(when)(lambda make=make: make().wait_send())


def line_sems(depth):
    dma = pltpu.SemaphoreType.DMA
    return [dma((2, depth))] * 4 + [dma((2, 2, depth))] * 2


def kernel(
    n, t, x_hbm, cq_hbm, cv_hbm, qf_hbm, vf_hbm, qw_hbm, vw_hbm, q1_hbm, q2_hbm, v1_hbm, v2_hbm,
    w_all, f_all, bits, grad,
    x, cq, cv, qf, vf, qw, vw, q1, q2, v1, v2,
    f_own, w_own, g, gc_in, gs, gy_in, gt, gz_in, u_own, u_all, u_flat, sq, sq_in,
    acc_q, acc_v, local, gsem, tsem, *sems):
    p = Place(n, t)
    depth = p.depth
    rows = q1.shape[0]
    rank, q_cols = acc_q.shape
    v_cols = acc_v.shape[1]
    F = Gather(p, f_own, f_all, sems[0:6])
    W = Line(p, w_own, w_all, sems[6:12])
    U = Gather(p, u_own, u_all, sems[12:18])
    pairs = (
        (qf_hbm, qf), (vf_hbm, vf), (qw_hbm, qw), (vw_hbm, vw), (x_hbm, x), (cq_hbm, cq), (cv_hbm, cv),
        (q1_hbm, q1), (q2_hbm, q2), (v1_hbm, v1), (v2_hbm, v2))
    loads = [pltpu.make_async_copy(src, dst, local.at[i]) for i, (src, dst) in enumerate(pairs)]
    for copy in loads:
        copy.start()

    barrier = pltpu.get_barrier_semaphore()
    peers = [{"fs": p.at(p.up(k), p.y, p.c)} for k in range(1, depth)]
    peers += [{"fs": p.at(p.z, 1 - p.y, p.c)}, {"fs": p.at(p.z, p.y, 1 - p.c)}]
    peers += [{"tp": (p.tp + k) % t} for k in range(1, t)]
    for peer in peers:
        pl.semaphore_signal(barrier, inc=1, device_id=peer, device_id_type=pl.DeviceIdType.MESH)
    loads[0].wait()
    loads[1].wait()
    f_own[:, :rank] = qf[...]
    f_own[:, rank:] = vf[...]
    pl.semaphore_wait(barrier, len(peers))

    for k in range(1, depth):
        F.send_z(k)
    F.send_yc(0)
    f_all[p.me] = f_own[...]
    loads[2].wait()
    loads[3].wait()
    w_own[:, :q_cols] = qw[...].astype(jnp.bfloat16)
    w_own[:, q_cols:] = vw[...].astype(jnp.bfloat16)
    w_all[p.me] = w_own[...]
    for k in range(1, depth):
        F.wait_z(k)
        F.send_yc(k)
    W.own_yc()
    W.send(0)
    for k in range(depth):
        F.pass_y(k)
    F.wait_c()
    for copy in loads[4:]:
        copy.wait()

    acc_q[...] = jnp.zeros_like(acc_q)
    acc_v[...] = jnp.zeros_like(acc_v)
    tile = 256

    @pl.loop(0, x.shape[0] // tile)
    def _(i):
        at = pl.ds(pl.multiple_of(i * tile, tile), tile)
        f = f_all[...].reshape(x.shape[1], 2 * rank)
        proj = jnp.dot(x[at, :], f, preferred_element_type=jnp.float32)
        turned = proj.T.astype(jnp.bfloat16)
        acc_q[...] += jnp.dot(turned[:rank], cq[at, :], preferred_element_type=jnp.float32)
        acc_v[...] += jnp.dot(turned[rank:], cv[at, :], preferred_element_type=jnp.float32)

    for j in range(n):
        c, y, z = j % CORES, (j // CORES) % COLS, j // (CORES * COLS)
        g[c, y, z, :, :q_cols] = acc_q[j * rows:(j + 1) * rows, :]
        g[c, y, z, :, q_cols:] = acc_v[j * rows:(j + 1) * rows, :]

    def swap(src, dst, k, peer):
        return pltpu.make_async_remote_copy(
            src_ref=src, dst_ref=dst, send_sem=gsem.at[0, k], recv_sem=gsem.at[1, k],
            device_id=peer, device_id_type=pl.DeviceIdType.MESH)

    to_core = swap(g.at[1 - p.c], gc_in, 0, {"fs": p.at(p.z, p.y, 1 - p.c)})
    to_core.start()
    W.wait(0)
    W.send(1)
    to_core.wait()
    gs[...] = g[p.c] + gc_in[...]
    to_col = swap(gs.at[1 - p.y], gy_in, depth, {"fs": p.at(p.z, 1 - p.y, p.c)})
    to_col.start()
    W.forward(0, 0)
    W.forward(1, 0, p.z == 0)
    to_col.wait()
    gt[...] = gs[p.y] + gy_in[...]
    to_z = [swap(gt.at[p.up(k)], gz_in.at[k - 1], k, {"fs": p.at(p.up(k), p.y, p.c)}) for k in range(1, depth)]
    for copy in to_z:
        copy.start()
    total = gt[p.z]
    for k, copy in enumerate(to_z):
        copy.wait()
        total = total + gz_in[k]
    grad[...] = total
    u_own[:, :q_cols] = moments(q1[...], q2[...], total[:, :q_cols])[2]
    u_own[:, q_cols:] = moments(v1[...], v2[...], total[:, q_cols:])[2]
    for k in range(1, depth):
        U.send_z(k)
    U.send_yc(0)
    for s in range(1, depth - 2):
        W.wait(s)
        W.send(s + 1)
        if s == 1:
            u_all[p.me] = u_own[...]
            for k in range(1, depth):
                U.wait_z(k)
                U.send_yc(k)
            W.forward(1, 0, p.z > 0)
        for d in range(2):
            W.forward(d, s)
    for k in range(depth):
        U.pass_y(k)
    U.wait_c()
    for j in range(n):
        u_flat[j * rows:(j + 1) * rows, :] = u_all[j]
    own_sq = jnp.sum(u_flat[...] * u_flat[...])
    sq[...] = jnp.full(sq.shape, own_sq, jnp.float32)
    shares = [
        pltpu.make_async_remote_copy(
            src_ref=sq, dst_ref=sq_in.at[k - 1], send_sem=tsem.at[0, k], recv_sem=tsem.at[1, k],
            device_id={"tp": (p.tp + k) % t}, device_id_type=pl.DeviceIdType.MESH)
        for k in range(1, t)
    ]
    for copy in shares:
        copy.start()
    W.wait(depth - 2)
    for d in range(2):
        W.forward(d, depth - 2)
    norm = sq[...]
    for k, copy in enumerate(shares):
        copy.wait()
        norm = norm + sq_in[k]
    entries = rank * (q_cols + v_cols) * t
    scale = lax.rsqrt(norm[:1, :1] / entries + 1e-06)
    bits[...] = (scale * u_flat[...]).astype(jnp.bfloat16)
    W.pass_y()
    W.wait_c()
    F.drain()
    U.drain()
    W.drain()


def exchange(*args):
    inputs, query_cot, value_cot, query_factor, value_factor, query_weight, value_weight = args[:7]
    n, t = lax.axis_size("fs"), lax.axis_size("tp")
    depth = n // (COLS * CORES)
    rows, q_cols = args[7].shape
    v_cols = args[9].shape[1]
    cols = q_cols + v_cols
    rank, deep = rows * n, query_factor.shape[0]
    any_, vmem = pl.BlockSpec(memory_space=pl.ANY), pl.BlockSpec(memory_space=pltpu.VMEM)
    f32, bf16 = jnp.float32, jnp.bfloat16
    dma = pltpu.SemaphoreType.DMA
    shape = jax.ShapeDtypeStruct
    w_all, f_all, bits, grad = pl.pallas_call(
        functools.partial(kernel, n, t),
        out_shape=(
            shape((n, deep, cols), bf16), shape((n, deep, 2 * rank), bf16), shape((rank, cols), bf16),
            shape((rows, cols), f32),
        ),
        in_specs=[any_] * len(args),
        out_specs=(vmem,) * 4,
        scratch_shapes=[pltpu.VMEM(a.shape, a.dtype) for a in args] + [
            pltpu.VMEM((deep, 2 * rank), bf16), pltpu.VMEM((deep, cols), bf16),
            pltpu.VMEM((CORES, COLS, depth, rows, cols), f32), pltpu.VMEM((COLS, depth, rows, cols), f32),
            pltpu.VMEM((COLS, depth, rows, cols), f32), pltpu.VMEM((depth, rows, cols), f32),
            pltpu.VMEM((depth, rows, cols), f32), pltpu.VMEM((depth - 1, rows, cols), f32),
            pltpu.VMEM((rows, cols), f32), pltpu.VMEM((n, rows, cols), f32), pltpu.VMEM((rank, cols), f32),
            pltpu.VMEM((8, 128), f32), pltpu.VMEM((t - 1, 8, 128), f32),
            pltpu.VMEM((rank, q_cols), f32), pltpu.VMEM((rank, v_cols), f32),
            dma((len(args),)), dma((2, depth + 1)), dma((2, t)),
        ] + gather_sems(depth) + line_sems(depth) + gather_sems(depth),
        compiler_params=pltpu.CompilerParams(
            collective_id=0, has_side_effects=True, vmem_limit_bytes=52 * 1024 * 1024),
    )(*args)
    first_q, second_q, _ = moments(args[7], args[8], grad[:, :q_cols])
    first_v, second_v, _ = moments(args[9], args[10], grad[:, q_cols:])
    return w_all, f_all, bits, first_q, second_q, first_v, second_v


def by_collectives(
    inputs, query_cot, value_cot, query_factor, value_factor, query_weight, value_weight,
    query_first, query_second, value_first, value_second,
):
    f_own = jnp.concatenate([query_factor, value_factor], axis=1)
    w_own = jnp.concatenate([query_weight, value_weight], axis=1).astype(jnp.bfloat16)
    q_cols = query_cot.shape[1]
    n, rank = lax.axis_size("fs"), f_own.shape[1] // 2
    entries = rank * (q_cols + value_cot.shape[1]) * lax.axis_size("tp")
    f_all = lax.all_gather(f_own, "fs", axis=0)
    w_all = lax.all_gather(w_own, "fs", axis=0)
    proj = jnp.dot(inputs, f_all.reshape(-1, 2 * rank), preferred_element_type=jnp.float32).astype(jnp.bfloat16)
    over = (((0,), (0,)), ((), ()))
    term_q = lax.dot_general(proj[:, :rank], query_cot, over, preferred_element_type=jnp.float32)
    term_v = lax.dot_general(proj[:, rank:], value_cot, over, preferred_element_type=jnp.float32)
    own = lax.psum_scatter(jnp.concatenate([term_q, term_v], axis=1), "fs", scatter_dimension=0, tiled=True)
    first_q, second_q, unit_q = moments(query_first, query_second, own[:, :q_cols])
    first_v, second_v, unit_v = moments(value_first, value_second, own[:, q_cols:])
    total = lax.psum(jnp.sum(unit_q * unit_q) + jnp.sum(unit_v * unit_v), ("fs", "tp"))
    scale = lax.rsqrt(total / entries + 1e-06)
    mine = (scale * jnp.concatenate([unit_q, unit_v], axis=1)).astype(jnp.bfloat16)
    bits = lax.all_gather(mine, "fs", axis=0, tiled=True)
    return w_all, f_all, bits, first_q, second_q, first_v, second_v


def on_device(
    inputs, query_cot, value_cot, query_factor, value_factor, query_weight, value_weight,
    query_first, query_second, value_first, value_second,
):
    n = lax.axis_size("fs")
    rank, q_cols, v_cols = query_factor.shape[1], query_cot.shape[1], value_cot.shape[1]
    whole = (
        n % (COLS * CORES) == 0 and n >= 4 * COLS * CORES and lax.axis_size("tp") > 1 and q_cols % 128 == 0
        and v_cols % 128 == 0 and (2 * rank) % 128 == 0 and inputs.shape[1] % 128 == 0
        and inputs.shape[0] % 256 == 0 and query_factor.shape[0] % 16 == 0 and rank % 16 == 0
    )
    run = exchange if whole else by_collectives
    w_all, f_all, bits, first_q, second_q, first_v, second_v = run(
        inputs, query_cot, value_cot, query_factor, value_factor, query_weight, value_weight,
        query_first, query_second, value_first, value_second)
    f_full = f_all.reshape(-1, 2 * rank)
    w_full = w_all.reshape(-1, q_cols + v_cols)
    bits_q, bits_v = bits[:, :q_cols], bits[:, q_cols:]
    f32 = jnp.float32
    step_q = jnp.dot(query_factor, bits_q, preferred_element_type=f32)
    step_v = jnp.dot(value_factor, bits_v, preferred_element_type=f32)
    new_q = query_weight - learn_rate * step_q
    new_v = value_weight - learn_rate * step_v
    all_q = jnp.dot(f_full[:, :rank], bits_q, preferred_element_type=f32)
    all_v = jnp.dot(f_full[:, rank:], bits_v, preferred_element_type=f32)
    copy_q = (w_full[:, :q_cols].astype(f32) - learn_rate * all_q).astype(jnp.bfloat16)
    copy_v = (w_full[:, q_cols:].astype(f32) - learn_rate * all_v).astype(jnp.bfloat16)
    return (step_q, step_v, new_q, new_v, first_q, second_q, first_v, second_v, copy_q, copy_v)


def solution(mesh):
    row, both = P("fs", None), P("fs", "tp")
    in_specs = (row, both, both, row, row) + (both,) * 6
    out_specs = (both,) * 8 + (P(None, "tp"),) * 2
    return jax.shard_map(on_device, mesh=mesh, in_specs=in_specs, out_specs=out_specs, check_vma=False)
```

```python
import functools

import jax
import jax.numpy as jnp
from jax import lax
from jax.experimental import pallas as pl
from jax.experimental.pallas import tpu as pltpu
from jax.sharding import PartitionSpec as P

first_decay = 0.9
second_decay = 0.99
small_eps = 1e-08
learn_rate = 0.01
CORES = 2
COLS = 2


def moments(old_first, old_second, gradient):
    first = first_decay * old_first + (1.0 - first_decay) * gradient
    second = second_decay * old_second + (1.0 - second_decay) * gradient * gradient
    unit = first / (jnp.sqrt(second) + small_eps)
    return (first, second, unit)


class Place:
    def __init__(self, n, t):
        self.n, self.t = n, t
        self.depth = n // (COLS * CORES)
        self.me = lax.axis_index("fs")
        self.tp = lax.axis_index("tp")
        self.c = self.me % CORES
        self.y = (self.me // CORES) % COLS
        self.z = self.me // (CORES * COLS)

    def at(self, z, y, c):
        return (z * COLS + y) * CORES + c

    def up(self, k):
        return (self.z + k) % self.depth

    def down(self, k):
        return (self.z + self.depth - k) % self.depth


class Gather:
    def __init__(self, place, own, full, sems):
        self.p, self.own, self.full = place, own, full
        self.zs, self.zr, self.ys, self.yr, self.cs, self.cr = sems
        self.sent = []

    def _copy(self, src, slot, ss, rs, to):
        return pltpu.make_async_remote_copy(
            src_ref=src, dst_ref=self.full.at[slot], send_sem=ss, recv_sem=rs,
            device_id={"fs": to}, device_id_type=pl.DeviceIdType.MESH)

    def _go(self, copy):
        copy.start()
        self.sent.append(copy)

    def piece(self, k):
        slot = self.p.at(self.p.down(k), self.p.y, self.p.c)
        return slot, (self.own if k == 0 else self.full.at[slot])

    def send_z(self, k):
        p = self.p
        self._go(self._copy(self.own, p.me, self.zs.at[k], self.zr.at[k], p.at(p.up(k), p.y, p.c)))

    def wait_z(self, k):
        slot = self.p.at(self.p.down(k), self.p.y, self.p.c)
        self._copy(self.full.at[slot], slot, self.zs.at[k], self.zr.at[k], self.p.me).wait_recv()

    def send_yc(self, k):
        p = self.p
        slot, src = self.piece(k)
        self._go(self._copy(src, slot, self.ys.at[k], self.yr.at[k], p.at(p.z, 1 - p.y, p.c)))
        self._go(self._copy(src, slot, self.cs.at[0, k], self.cr.at[0, k], p.at(p.z, p.y, 1 - p.c)))

    def pass_y(self, k):
        p = self.p
        slot = p.at(p.down(k), 1 - p.y, p.c)
        got = self.full.at[slot]
        self._copy(got, slot, self.ys.at[k], self.yr.at[k], p.me).wait_recv()
        self._go(self._copy(got, slot, self.cs.at[1, k], self.cr.at[1, k], p.at(p.z, p.y, 1 - p.c)))

    def wait_c(self):
        p = self.p
        for j in range(2):
            for k in range(p.depth):
                slot = p.at(p.down(k), p.y if j == 0 else 1 - p.y, 1 - p.c)
                self._copy(self.full.at[slot], slot, self.cs.at[j, k], self.cr.at[j, k], p.me).wait_recv()

    def drain(self):
        for copy in self.sent:
            copy.wait_send()


def gather_sems(depth):
    dma = pltpu.SemaphoreType.DMA
    return [dma((depth,)), dma((depth,)), dma((depth,)), dma((depth,)), dma((2, depth)), dma((2, depth))]


class Line:
    def __init__(self, place, own, full, sems):
        self.p, self.own, self.full = place, own, full
        self.zs, self.zr, self.ys, self.yr, self.cs, self.cr = sems
        self.sent = []

    def _copy(self, src, slot, ss, rs, to):
        return pltpu.make_async_remote_copy(
            src_ref=src, dst_ref=self.full.at[slot], send_sem=ss, recv_sem=rs,
            device_id={"fs": to}, device_id_type=pl.DeviceIdType.MESH)

    def _go(self, when, make):
        pl.when(when)(lambda: make().start())
        self.sent.append((when, make))

    def origin(self, d, s):
        z = self.p.z - 1 - s if d == 0 else self.p.z + 1 + s
        return z, (z >= 0 if d == 0 else z < self.p.depth)

    def send(self, s):
        p = self.p
        for d in range(2):
            to, frm = (p.z + 1, p.z - s) if d == 0 else (p.z - 1, p.z + s)
            when = jnp.logical_and(to < p.depth, frm >= 0) if d == 0 else jnp.logical_and(to >= 0, frm < p.depth)

            def make(d=d, to=to, frm=frm):
                slot = p.at(frm, p.y, p.c)
                src = self.own if s == 0 else self.full.at[slot]
                return self._copy(src, slot, self.zs.at[d, s], self.zr.at[d, s], p.at(to, p.y, p.c))

            self._go(when, make)

    def wait(self, s):
        p = self.p
        for d in range(2):
            z, when = self.origin(d, s)

            @pl.when(when)
            def _(d=d, z=z):
                slot = p.at(z, p.y, p.c)
                self._copy(self.full.at[slot], slot, self.zs.at[d, s], self.zr.at[d, s], p.me).wait_recv()

    def own_yc(self):
        p, k = self.p, self.p.depth - 1
        self._go(True, lambda: self._copy(
            self.own, p.me, self.ys.at[0, k], self.yr.at[0, k], p.at(p.z, 1 - p.y, p.c)))
        self._go(True, lambda: self._copy(
            self.own, p.me, self.cs.at[0, 0, k], self.cr.at[0, 0, k], p.at(p.z, p.y, 1 - p.c)))

    def forward(self, d, s, also=True):
        p = self.p
        z, when = self.origin(d, s)
        when = jnp.logical_and(when, also)

        def to_y():
            slot = p.at(z, p.y, p.c)
            return self._copy(self.full.at[slot], slot, self.ys.at[d, s], self.yr.at[d, s], p.at(p.z, 1 - p.y, p.c))

        def to_c():
            slot = p.at(z, p.y, p.c)
            return self._copy(
                self.full.at[slot], slot, self.cs.at[0, d, s], self.cr.at[0, d, s], p.at(p.z, p.y, 1 - p.c))

        self._go(when, to_y)
        self._go(when, to_c)

    def items(self):
        last = self.p.depth - 1
        yield 0, last, self.p.z, True
        for s in range(last):
            for d in range(2):
                z, when = self.origin(d, s)
                yield d, s, z, when

    def pass_y(self):
        p = self.p
        for d, s, z, when in self.items():
            slot = p.at(z, 1 - p.y, p.c)

            @pl.when(when)
            def _(d=d, s=s, slot=slot):
                got = self.full.at[slot]
                self._copy(got, slot, self.ys.at[d, s], self.yr.at[d, s], p.me).wait_recv()

            self._go(when, lambda d=d, s=s, slot=slot: self._copy(
                self.full.at[slot], slot, self.cs.at[1, d, s], self.cr.at[1, d, s], p.at(p.z, p.y, 1 - p.c)))

    def wait_c(self):
        p = self.p
        for j in range(2):
            for d, s, z, when in self.items():
                slot = p.at(z, p.y if j == 0 else 1 - p.y, 1 - p.c)

                @pl.when(when)
                def _(d=d, s=s, slot=slot):
                    self._copy(self.full.at[slot], slot, self.cs.at[j, d, s], self.cr.at[j, d, s], p.me).wait_recv()

    def drain(self):
        for when, make in self.sent:
            pl.when(when)(lambda make=make: make().wait_send())


def line_sems(depth):
    dma = pltpu.SemaphoreType.DMA
    return [dma((2, depth))] * 4 + [dma((2, 2, depth))] * 2


def kernel(
    n, t, x_hbm, cq_hbm, cv_hbm, qf_hbm, vf_hbm, qw_hbm, vw_hbm, q1_hbm, q2_hbm, v1_hbm, v2_hbm,
    w_all, f_all, bits, grad,
    x, cq, cv, qf, vf, qw, vw, q1, q2, v1, v2,
    f_own, w_own, g, gc_in, gs, gy_in, gt, gz_in, u_own, u_all, u_flat, sq, sq_in,
    acc_q, acc_v, local, gsem, tsem, *sems):
    p = Place(n, t)
    depth = p.depth
    rows = q1.shape[0]
    rank, q_cols = acc_q.shape
    v_cols = acc_v.shape[1]
    F = Gather(p, f_own, f_all, sems[0:6])
    W = Line(p, w_own, w_all, sems[6:12])
    U = Gather(p, u_own, u_all, sems[12:18])
    pairs = (
        (qf_hbm, qf), (vf_hbm, vf), (qw_hbm, qw), (vw_hbm, vw), (x_hbm, x), (cq_hbm, cq), (cv_hbm, cv),
        (q1_hbm, q1), (q2_hbm, q2), (v1_hbm, v1), (v2_hbm, v2))
    loads = [pltpu.make_async_copy(src, dst, local.at[i]) for i, (src, dst) in enumerate(pairs)]
    for copy in loads:
        copy.start()

    barrier = pltpu.get_barrier_semaphore()
    peers = [{"fs": p.at(p.up(k), p.y, p.c)} for k in range(1, depth)]
    peers += [{"fs": p.at(p.z, 1 - p.y, p.c)}, {"fs": p.at(p.z, p.y, 1 - p.c)}]
    peers += [{"tp": (p.tp + k) % t} for k in range(1, t)]
    for peer in peers:
        pl.semaphore_signal(barrier, inc=1, device_id=peer, device_id_type=pl.DeviceIdType.MESH)
    loads[0].wait()
    loads[1].wait()
    f_own[:, :rank] = qf[...]
    f_own[:, rank:] = vf[...]
    pl.semaphore_wait(barrier, len(peers))

    for k in range(1, depth):
        F.send_z(k)
    F.send_yc(0)
    f_all[p.me] = f_own[...]
    loads[2].wait()
    loads[3].wait()
    w_own[:, :q_cols] = qw[...].astype(jnp.bfloat16)
    w_own[:, q_cols:] = vw[...].astype(jnp.bfloat16)
    w_all[p.me] = w_own[...]
    for k in range(1, depth):
        F.wait_z(k)
        F.send_yc(k)
    W.own_yc()
    W.send(0)
    for k in range(depth):
        F.pass_y(k)
    F.wait_c()
    for copy in loads[4:]:
        copy.wait()

    acc_q[...] = jnp.zeros_like(acc_q)
    acc_v[...] = jnp.zeros_like(acc_v)
    tile = 256

    @pl.loop(0, x.shape[0] // tile)
    def _(i):
        at = pl.ds(pl.multiple_of(i * tile, tile), tile)
        f = f_all[...].reshape(x.shape[1], 2 * rank)
        proj = jnp.dot(x[at, :], f, preferred_element_type=jnp.float32)
        turned = proj.T.astype(jnp.bfloat16)
        acc_q[...] += jnp.dot(turned[:rank], cq[at, :], preferred_element_type=jnp.float32)
        acc_v[...] += jnp.dot(turned[rank:], cv[at, :], preferred_element_type=jnp.float32)

    for j in range(n):
        c, y, z = j % CORES, (j // CORES) % COLS, j // (CORES * COLS)
        g[c, y, z, :, :q_cols] = acc_q[j * rows:(j + 1) * rows, :]
        g[c, y, z, :, q_cols:] = acc_v[j * rows:(j + 1) * rows, :]

    def swap(src, dst, k, peer):
        return pltpu.make_async_remote_copy(
            src_ref=src, dst_ref=dst, send_sem=gsem.at[0, k], recv_sem=gsem.at[1, k],
            device_id=peer, device_id_type=pl.DeviceIdType.MESH)

    to_core = swap(g.at[1 - p.c], gc_in, 0, {"fs": p.at(p.z, p.y, 1 - p.c)})
    to_core.start()
    W.wait(0)
    W.send(1)
    to_core.wait()
    gs[...] = g[p.c] + gc_in[...]
    to_col = swap(gs.at[1 - p.y], gy_in, depth, {"fs": p.at(p.z, 1 - p.y, p.c)})
    to_col.start()
    W.forward(0, 0)
    W.forward(1, 0, p.z == 0)
    to_col.wait()
    gt[...] = gs[p.y] + gy_in[...]
    to_z = [swap(gt.at[p.up(k)], gz_in.at[k - 1], k, {"fs": p.at(p.up(k), p.y, p.c)}) for k in range(1, depth)]
    for copy in to_z:
        copy.start()
    total = gt[p.z]
    for k, copy in enumerate(to_z):
        copy.wait()
        total = total + gz_in[k]
    grad[...] = total
    u_own[:, :q_cols] = moments(q1[...], q2[...], total[:, :q_cols])[2]
    u_own[:, q_cols:] = moments(v1[...], v2[...], total[:, q_cols:])[2]
    for k in range(1, depth):
        U.send_z(k)
    U.send_yc(0)
    for s in range(1, depth - 2):
        W.wait(s)
        W.send(s + 1)
        if s == 1:
            u_all[p.me] = u_own[...]
            for k in range(1, depth):
                U.wait_z(k)
                U.send_yc(k)
            W.forward(1, 0, p.z > 0)
        for d in range(2):
            W.forward(d, s)
    for k in range(depth):
        U.pass_y(k)
    U.wait_c()
    for j in range(n):
        u_flat[j * rows:(j + 1) * rows, :] = u_all[j]
    own_sq = jnp.sum(u_flat[...] * u_flat[...])
    sq[...] = jnp.full(sq.shape, own_sq, jnp.float32)
    shares = [
        pltpu.make_async_remote_copy(
            src_ref=sq, dst_ref=sq_in.at[k - 1], send_sem=tsem.at[0, k], recv_sem=tsem.at[1, k],
            device_id={"tp": (p.tp + k) % t}, device_id_type=pl.DeviceIdType.MESH)
        for k in range(1, t)
    ]
    for copy in shares:
        copy.start()
    W.wait(depth - 2)
    for d in range(2):
        W.forward(d, depth - 2)
    norm = sq[...]
    for k, copy in enumerate(shares):
        copy.wait()
        norm = norm + sq_in[k]
    entries = rank * (q_cols + v_cols) * t
    scale = lax.rsqrt(norm[:1, :1] / entries + 1e-06)
    bits[...] = (scale * u_flat[...]).astype(jnp.bfloat16)
    W.pass_y()
    W.wait_c()
    F.drain()
    U.drain()
    W.drain()


def exchange(*args):
    inputs, query_cot, value_cot, query_factor, value_factor, query_weight, value_weight = args[:7]
    n, t = lax.axis_size("fs"), lax.axis_size("tp")
    depth = n // (COLS * CORES)
    rows, q_cols = args[7].shape
    v_cols = args[9].shape[1]
    cols = q_cols + v_cols
    rank, deep = rows * n, query_factor.shape[0]
    any_, vmem = pl.BlockSpec(memory_space=pl.ANY), pl.BlockSpec(memory_space=pltpu.VMEM)
    f32, bf16 = jnp.float32, jnp.bfloat16
    dma = pltpu.SemaphoreType.DMA
    shape = jax.ShapeDtypeStruct
    w_all, f_all, bits, grad = pl.pallas_call(
        functools.partial(kernel, n, t),
        out_shape=(
            shape((n, deep, cols), bf16), shape((n, deep, 2 * rank), bf16), shape((rank, cols), bf16),
            shape((rows, cols), f32),
        ),
        in_specs=[any_] * len(args),
        out_specs=(vmem,) * 4,
        scratch_shapes=[pltpu.VMEM(a.shape, a.dtype) for a in args] + [
            pltpu.VMEM((deep, 2 * rank), bf16), pltpu.VMEM((deep, cols), bf16),
            pltpu.VMEM((CORES, COLS, depth, rows, cols), f32), pltpu.VMEM((COLS, depth, rows, cols), f32),
            pltpu.VMEM((COLS, depth, rows, cols), f32), pltpu.VMEM((depth, rows, cols), f32),
            pltpu.VMEM((depth, rows, cols), f32), pltpu.VMEM((depth - 1, rows, cols), f32),
            pltpu.VMEM((rows, cols), f32), pltpu.VMEM((n, rows, cols), f32), pltpu.VMEM((rank, cols), f32),
            pltpu.VMEM((8, 128), f32), pltpu.VMEM((t - 1, 8, 128), f32),
            pltpu.VMEM((rank, q_cols), f32), pltpu.VMEM((rank, v_cols), f32),
            dma((len(args),)), dma((2, depth + 1)), dma((2, t)),
        ] + gather_sems(depth) + line_sems(depth) + gather_sems(depth),
        compiler_params=pltpu.CompilerParams(
            collective_id=0, has_side_effects=True, vmem_limit_bytes=54 * 1024 * 1024 - 65536),
    )(*args)
    first_q, second_q, _ = moments(args[7], args[8], grad[:, :q_cols])
    first_v, second_v, _ = moments(args[9], args[10], grad[:, q_cols:])
    return w_all, f_all, bits, first_q, second_q, first_v, second_v


def by_collectives(
    inputs, query_cot, value_cot, query_factor, value_factor, query_weight, value_weight,
    query_first, query_second, value_first, value_second,
):
    f_own = jnp.concatenate([query_factor, value_factor], axis=1)
    w_own = jnp.concatenate([query_weight, value_weight], axis=1).astype(jnp.bfloat16)
    q_cols = query_cot.shape[1]
    n, rank = lax.axis_size("fs"), f_own.shape[1] // 2
    entries = rank * (q_cols + value_cot.shape[1]) * lax.axis_size("tp")
    f_all = lax.all_gather(f_own, "fs", axis=0)
    w_all = lax.all_gather(w_own, "fs", axis=0)
    proj = jnp.dot(inputs, f_all.reshape(-1, 2 * rank), preferred_element_type=jnp.float32).astype(jnp.bfloat16)
    over = (((0,), (0,)), ((), ()))
    term_q = lax.dot_general(proj[:, :rank], query_cot, over, preferred_element_type=jnp.float32)
    term_v = lax.dot_general(proj[:, rank:], value_cot, over, preferred_element_type=jnp.float32)
    own = lax.psum_scatter(jnp.concatenate([term_q, term_v], axis=1), "fs", scatter_dimension=0, tiled=True)
    first_q, second_q, unit_q = moments(query_first, query_second, own[:, :q_cols])
    first_v, second_v, unit_v = moments(value_first, value_second, own[:, q_cols:])
    total = lax.psum(jnp.sum(unit_q * unit_q) + jnp.sum(unit_v * unit_v), ("fs", "tp"))
    scale = lax.rsqrt(total / entries + 1e-06)
    mine = (scale * jnp.concatenate([unit_q, unit_v], axis=1)).astype(jnp.bfloat16)
    bits = lax.all_gather(mine, "fs", axis=0, tiled=True)
    return w_all, f_all, bits, first_q, second_q, first_v, second_v


def copy_kernel(w, f, bits, copy_q, copy_v):
    rank, q_cols = f.shape[2] // 2, copy_q.shape[1]
    for i in range(w.shape[0]):
        deep = w.shape[1]
        at = slice(i * deep, (i + 1) * deep)
        step_q = jnp.dot(f[i][:, :rank], bits[:, :q_cols], preferred_element_type=jnp.float32)
        step_v = jnp.dot(f[i][:, rank:], bits[:, q_cols:], preferred_element_type=jnp.float32)
        copy_q[at, :] = (w[i][:, :q_cols].astype(jnp.float32) - learn_rate * step_q).astype(jnp.bfloat16)
        copy_v[at, :] = (w[i][:, q_cols:].astype(jnp.float32) - learn_rate * step_v).astype(jnp.bfloat16)


def copies(w_all, f_all, bits, q_cols):
    n, deep, cols = w_all.shape
    some = 2
    shape = jax.ShapeDtypeStruct
    return pl.pallas_call(
        copy_kernel,
        grid=(n // some,),
        out_shape=(shape((n * deep, q_cols), jnp.bfloat16), shape((n * deep, cols - q_cols), jnp.bfloat16)),
        in_specs=[
            pl.BlockSpec((some, deep, cols), lambda i: (i, 0, 0)),
            pl.BlockSpec((some,) + f_all.shape[1:], lambda i: (i, 0, 0)),
            pl.BlockSpec(bits.shape, lambda i: (0, 0)),
        ],
        out_specs=(
            pl.BlockSpec((some * deep, q_cols), lambda i: (i, 0)),
            pl.BlockSpec((some * deep, cols - q_cols), lambda i: (i, 0)),
        ),
    )(w_all, f_all, bits)


def on_device(
    inputs, query_cot, value_cot, query_factor, value_factor, query_weight, value_weight,
    query_first, query_second, value_first, value_second,
):
    n = lax.axis_size("fs")
    rank, q_cols, v_cols = query_factor.shape[1], query_cot.shape[1], value_cot.shape[1]
    whole = (
        n % (COLS * CORES) == 0 and n >= 4 * COLS * CORES and lax.axis_size("tp") > 1 and q_cols % 128 == 0
        and v_cols % 128 == 0 and (2 * rank) % 128 == 0 and inputs.shape[1] % 128 == 0
        and inputs.shape[0] % 256 == 0 and query_factor.shape[0] % 16 == 0 and rank % 16 == 0
    )
    run = exchange if whole else by_collectives
    w_all, f_all, bits, first_q, second_q, first_v, second_v = run(
        inputs, query_cot, value_cot, query_factor, value_factor, query_weight, value_weight,
        query_first, query_second, value_first, value_second)
    if whole:
        step_q = jnp.dot(query_factor, bits[:, :q_cols], preferred_element_type=jnp.float32)
        step_v = jnp.dot(value_factor, bits[:, q_cols:], preferred_element_type=jnp.float32)
        new_q = query_weight - learn_rate * step_q
        new_v = value_weight - learn_rate * step_v
        copy_q, copy_v = copies(w_all, f_all, bits, q_cols)
        return (step_q, step_v, new_q, new_v, first_q, second_q, first_v, second_v, copy_q, copy_v)
    f_full = f_all.reshape(-1, 2 * rank)
    w_full = w_all.reshape(-1, q_cols + v_cols)
    bits_q, bits_v = bits[:, :q_cols], bits[:, q_cols:]
    f32 = jnp.float32
    step_q = jnp.dot(query_factor, bits_q, preferred_element_type=f32)
    step_v = jnp.dot(value_factor, bits_v, preferred_element_type=f32)
    new_q = query_weight - learn_rate * step_q
    new_v = value_weight - learn_rate * step_v
    all_q = jnp.dot(f_full[:, :rank], bits_q, preferred_element_type=f32)
    all_v = jnp.dot(f_full[:, rank:], bits_v, preferred_element_type=f32)
    copy_q = (w_full[:, :q_cols].astype(f32) - learn_rate * all_q).astype(jnp.bfloat16)
    copy_v = (w_full[:, q_cols:].astype(f32) - learn_rate * all_v).astype(jnp.bfloat16)
    return (step_q, step_v, new_q, new_v, first_q, second_q, first_v, second_v, copy_q, copy_v)


def solution(mesh):
    row, both = P("fs", None), P("fs", "tp")
    in_specs = (row, both, both, row, row) + (both,) * 6
    out_specs = (both,) * 8 + (P(None, "tp"),) * 2
    return jax.shard_map(on_device, mesh=mesh, in_specs=in_specs, out_specs=out_specs, check_vma=False)
```
